32 devices in a mesh: kv: 8 (over z, core), tp: 4 (over y, x).
Axes of the slice: x: 2, y: 2, z: 4, core: 2. Of those that a mesh axis runs over, the one named last changes fastest.
Arguments:
- tokens: bfloat16 [64, 4096], P(None, ('kv', 'tp')), may hold values from -3 to 3
- lengths: int32 [16], replicated, may hold values from 1 to 4, 32 in all
- states: float32 [16, 16, 128, 128], P('kv', 'tp'), may hold values from -3 to 3
- gain_pre: float32 [4096], P('kv'), may hold values from 0.1 to 1.9
- pre_gate: bfloat16 [4096, 11264], P('kv', 'tp'), may hold values from -0.09375 to 0.09375
- pre_up: bfloat16 [4096, 11264], P('kv', 'tp'), may hold values from -0.09375 to 0.09375
- pre_down: bfloat16 [11264, 4096], P('tp', 'kv'), may hold values from -1 to 1
- gain_mix: float32 [4096], P('kv'), may hold values from 0.1 to 1.9
- query_weight: bfloat16 [4096, 2048], P('kv', 'tp'), may hold values from -0.09375 to 0.09375
- forget_weight: bfloat16 [4096, 2048], P('kv', 'tp'), may hold values from -0.09375 to 0.09375
- input_weight: bfloat16 [4096, 2048], P('kv', 'tp'), may hold values from -0.09375 to 0.09375
- outgate_weight: bfloat16 [4096, 2048], P('kv', 'tp'), may hold values from -0.09375 to 0.09375
- forget_floor: float32 [2048], P('tp'), may hold values from 0 to 0.9
- head_gain: float32 [128], replicated, may hold values from 0.1 to 1.9
- mix_weight: bfloat16 [2048, 4096], P('tp', 'kv'), may hold values from -1 to 1
- gain_post: float32 [4096], P('kv'), may hold values from 0.1 to 1.9
- post_gate: bfloat16 [4096, 11264], P('kv', 'tp'), may hold values from -0.09375 to 0.09375
- post_up: bfloat16 [4096, 11264], P('kv', 'tp'), may hold values from -0.09375 to 0.09375
- post_down: bfloat16 [11264, 4096], P('tp', 'kv'), may hold values from -0.0546875 to 0.0546875
Outputs:
- out_tokens: bfloat16 [64, 4096], P(None, ('kv', 'tp'))
- new_states: float32 [16, 16, 128, 128], P('kv', 'tp')
The draws below stay inside these ranges and needn't reach their ends.
Inputs may be any that keep to these rules, and one draw needn't show every extreme that they name: `lengths`: each of the 16 sequences has 1 to 4 new tokens, 32 in all, and at least one has exactly 4.
All inputs are finite; a program needn't handle non-finite values.
Results may differ from the reference program's by a relative error of at most 0.011.
Values may be sent and summed in bfloat16 or wider, within the bound.
A program may use at most 64 MiB of HBM per device.

```python
import math
import jax
import jax.numpy as jnp
import numpy as np
from jax import lax

D = 4096
FF = 11264
HEADS = 16
DK = 128
W = 4
BATCH = 16
ROWS = 64
HW = 2048


def draw_tokens(key, part):
    noise_key = jax.random.fold_in(key, 11)
    phase_key = jax.random.fold_in(key, 12)
    shrink_key = jax.random.fold_in(key, 14)
    columns = jnp.arange(D, dtype=jnp.float32) / D
    phase_shift = jax.random.uniform(phase_key, (), jnp.float32, 0.0, 6.283)
    profile = jnp.exp(1.2 * jnp.cos(6.283 * columns + phase_shift))
    shrink = jnp.exp(jax.random.uniform(shrink_key, (ROWS, 1), jnp.float32, -4.0, -2.0))
    samples = jnp.clip(jax.random.normal(noise_key, (ROWS, D), jnp.float32), -6.0, 6.0)
    return (samples * profile[None, :] * shrink).astype(jnp.bfloat16)


def column_levels(key, stream):
    level_key = jax.random.fold_in(key, stream)
    groups = D // 64
    exponents = jax.random.uniform(level_key, (groups,), jnp.float32, -1.5, 1.5)
    return jnp.repeat(jnp.exp(exponents), 64)


def draw_pre_down(key, part):
    noise_key = jax.random.fold_in(key, 21)
    samples = jnp.clip(jax.random.normal(noise_key, (FF, D), jnp.float32), -4.0, 4.0)
    levels = column_levels(key, 22)
    return (samples * levels[None, :] / jnp.sqrt(jnp.float32(FF))).astype(jnp.bfloat16)


def draw_mix_weight(key, part):
    noise_key = jax.random.fold_in(key, 31)
    samples = jnp.clip(jax.random.normal(noise_key, (HW, D), jnp.float32), -4.0, 4.0)
    levels = column_levels(key, 32)
    return (samples * levels[None, :] / jnp.sqrt(jnp.float32(HW))).astype(jnp.bfloat16)


def steps_of(stream_key, extent, shards, low, largest):
    level, own = 1.0, jax.random.fold_in(stream_key, 6)
    for axis_at, parts in shards:
        steps = jnp.exp(jax.random.uniform(jax.random.fold_in(own, axis_at), (parts,), jnp.float32, low / len(shards), largest / len(shards)))
        level = level * jnp.repeat(steps, extent[axis_at] // parts).reshape([-1 if axis == axis_at else 1 for axis in range(len(extent))])
    return level


def length_profile(count, total, reach, skew):
    portions = [(1 << 20) // math.isqrt(rank ** skew) + 1 for rank in range(2, count + 1)]
    surplus, given = total - reach - (count - 1), [1] * (count - 1)
    while surplus > 0:
        movable = [i for i in range(count - 1) if given[i] < reach]
        whole, budget = sum([portions[i] for i in movable]), surplus
        for i in movable:
            more = min(reach - given[i], max(1, budget * portions[i] // whole), surplus)
            given[i] = given[i] + more
            surplus = surplus - more
    return np.array([reach] + given)


def uneven(key, amount, total, reach, skew):
    if amount == 2:
        one = jax.random.randint(key, (), max(1, total - reach), min(reach, total - 1) + 1)
        return jnp.stack([one, total - one])
    sizes = jnp.asarray(length_profile(amount, total, reach, skew), jnp.int32)
    pairs = (amount - 1) // 2
    donor, receiver = sizes[1:1 + 2 * pairs:2], sizes[2:2 + 2 * pairs:2]
    room = jnp.minimum(donor - 1, reach - receiver)
    moved = jax.random.randint(jax.random.fold_in(key, 1), (pairs,), 0, 1 << 20) % (room + 1)
    sizes = sizes.at[1:1 + 2 * pairs:2].set(donor - moved).at[2:2 + 2 * pairs:2].set(receiver + moved)
    return sizes[jax.random.permutation(jax.random.fold_in(key, 2), amount)]


def noise(stream_key, dims, scale, reach, cuts=(), held_as=jnp.bfloat16):
    factor_of = steps_of(stream_key, dims, cuts, -0.22, 0.18) if cuts else 1.0
    drawn = jax.random.normal(stream_key, dims, jnp.float32) * scale * factor_of
    return jnp.minimum(jnp.maximum(drawn, -reach), reach).astype(held_as)


def setup_inputs(seed: int = 0) -> dict:
    keys = jax.random.split(jax.random.key(seed), 20)
    return {
        "tokens": draw_tokens(jax.random.fold_in(keys[19], 71), 0),
        "lengths": uneven(keys[1], BATCH, 2 * BATCH, W, 2).astype(jnp.int32),
        "states": noise(keys[2], (BATCH, HEADS, DK, DK), 0.5, 3.0, ((0, 8), (1, 4)), jnp.float32),
        "gain_pre": jnp.clip(1.0 + 0.18 * jax.random.normal(keys[3], (D,), jnp.float32), 0.1, 1.9),
        "pre_gate": noise(keys[4], (D, FF), D ** -0.5, 0.09375, ((0, 8), (1, 4))),
        "pre_up": noise(keys[5], (D, FF), D ** -0.5, 0.09375, ((0, 8), (1, 4))),
        "pre_down": draw_pre_down(jax.random.fold_in(keys[19], 71), 0),
        "gain_mix": jnp.clip(1.0 + 0.18 * jax.random.normal(keys[7], (D,), jnp.float32), 0.1, 1.9),
        "query_weight": noise(keys[8], (D, HW), D ** -0.5, 0.09375, ((0, 8), (1, 4))),
        "forget_weight": noise(keys[9], (D, HW), D ** -0.5, 0.09375, ((0, 8), (1, 4))),
        "input_weight": noise(keys[10], (D, HW), D ** -0.5, 0.09375, ((0, 8), (1, 4))),
        "outgate_weight": noise(keys[11], (D, HW), D ** -0.5, 0.09375, ((0, 8), (1, 4))),
        "forget_floor": jnp.clip(0.9 * jax.random.uniform(keys[12], (HW,), jnp.float32) ** steps_of(keys[12], (HW,), ((0, 4),), -0.2, 0.2), 0.0, 0.9),
        "head_gain": jnp.clip(1.0 + 0.18 * jax.random.normal(keys[13], (DK,), jnp.float32), 0.1, 1.9),
        "mix_weight": draw_mix_weight(jax.random.fold_in(keys[19], 71), 0),
        "gain_post": jnp.clip(1.0 + 0.18 * jax.random.normal(keys[15], (D,), jnp.float32), 0.1, 1.9),
        "post_gate": noise(keys[16], (D, FF), D ** -0.5, 0.09375, ((0, 8), (1, 4))),
        "post_up": noise(keys[17], (D, FF), D ** -0.5, 0.09375, ((0, 8), (1, 4))),
        "post_down": noise(keys[18], (FF, D), FF ** -0.5, 0.0546875, ((0, 4), (1, 8))),
    }


EPSILON = 1e-06

def normalize(values, gain):
    floats = values.astype(jnp.float32)
    meansq = lax.optimization_barrier(jnp.mean(floats * floats, axis=1, keepdims=True))
    return (floats * lax.rsqrt(meansq + EPSILON) * gain).astype(jnp.bfloat16)

def half_mixer(values, gain, gate_weight, up_weight, down_weight):
    normed = normalize(values, gain)
    gate_part = jnp.dot(normed, gate_weight, preferred_element_type=jnp.float32)
    up_part = jnp.dot(normed, up_weight, preferred_element_type=jnp.float32)
    hidden = (jax.nn.silu(gate_part) * up_part).astype(jnp.bfloat16)
    return jnp.dot(hidden, down_weight, preferred_element_type=jnp.float32)

def reference(tokens, lengths, states, gain_pre, pre_gate, pre_up, pre_down, gain_mix, query_weight, forget_weight, input_weight, outgate_weight, forget_floor, head_gain, mix_weight, gain_post, post_gate, post_up, post_down):
    resid_one = (tokens.astype(jnp.float32) + 0.5 * half_mixer(tokens, gain_pre, pre_gate, pre_up, pre_down)).astype(jnp.bfloat16)
    normed = normalize(resid_one, gain_mix)
    shape_four = (BATCH, W, HEADS, DK)
    queries = jax.nn.silu(jnp.dot(normed, query_weight, preferred_element_type=jnp.float32)).reshape(shape_four)
    forget_raw = jnp.dot(normed, forget_weight, preferred_element_type=jnp.float32).reshape(shape_four)
    fresh_values = jnp.dot(normed, input_weight, preferred_element_type=jnp.float32).reshape(shape_four)
    gating = jnp.dot(normed, outgate_weight, preferred_element_type=jnp.float32).reshape(shape_four)
    live_mask = jnp.arange(W, dtype=jnp.int32)[None, :] < lengths[:, None]
    live_four = live_mask[:, :, None, None]
    floors = forget_floor.reshape(HEADS, DK)
    forgets = jnp.where(live_four, floors + (1.0 - floors) * jax.nn.sigmoid(forget_raw), jnp.float32(1.0))
    write_rate = 1.0 - forgets
    carried = states
    readings = []
    for offset in range(W):
        carried = forgets[:, offset, :, :, None] * carried + write_rate[:, offset, :, :, None] * fresh_values[:, offset, :, None, :]
        readings.append(jnp.einsum('bhk,bhkv->bhv', queries[:, offset], carried, precision=lax.Precision.HIGHEST))
    read_out = jnp.stack(readings, axis=1)
    meansq = lax.optimization_barrier(jnp.mean(read_out * read_out, axis=3, keepdims=True))
    head_out = (read_out * lax.rsqrt(meansq + EPSILON) * head_gain * jax.nn.silu(gating) * live_four.astype(jnp.float32)).astype(jnp.bfloat16).reshape(BATCH * W, HEADS * DK)
    mixed = jnp.dot(head_out, mix_weight, preferred_element_type=jnp.float32)
    resid_two = (resid_one.astype(jnp.float32) + mixed).astype(jnp.bfloat16)
    live_rows = live_mask.reshape(BATCH * W, 1).astype(jnp.float32)
    outcome = ((resid_two.astype(jnp.float32) + 0.5 * half_mixer(resid_two, gain_post, post_gate, post_up, post_down)) * live_rows).astype(jnp.bfloat16)
    return (outcome, carried)
```

```python
import functools

import jax
import jax.numpy as jnp
from jax import lax
from jax.experimental import pallas as pl
from jax.experimental.pallas import tpu as pltpu
from jax.sharding import PartitionSpec as P

D = 4096
DK = 128
W = 4
EPSILON = 1e-06
MESH = pl.DeviceIdType.MESH
F32 = jnp.float32
BF16 = jnp.bfloat16
CORES = 2


def silu(v):
    return v / (1.0 + jnp.exp(-v))


def sigmoid(v):
    return 1.0 / (1.0 + jnp.exp(-v))


def kernel(cfg, *refs):
    NK, NT, C, FL, HL, ROWS, aligned, nch = cfg
    NZ = NK // CORES
    RL = ROWS // NK
    FC = FL // nch
    it = iter(refs)
    (tokens, lengths, states_h, g_pre, pg_h, pu_h, pd_h, g_mix, q_h, f_h, i_h, o_h, floor, head_gain, mw_h,
     g_post, sg_h, su_h, sd_h) = [next(it) for _ in range(19)]
    out, ns_h = next(it), next(it)
    (x0, x1, x2, wpg, wpu, wpd, wq, wmw, wsg, wsu, wsd, st, tok_s, tok_r, w_sem, st_sem) = [
        next(it) for _ in range(16)]
    sq_bufs = [[next(it) for _ in range(4)] for _ in range(3)]
    ffn_bufs = [[next(it) for _ in range(14)] for _ in range(2)]
    mix_bufs = [next(it) for _ in range(9)]
    hg_bufs = [next(it) for _ in range(3)]
    ro = next(it)
    ar_bufs = [[next(it) for _ in range(3)] for _ in range(3)]
    fin = [next(it) for _ in range(2)]

    k = lax.axis_index("kv")
    t = lax.axis_index("tp")
    z = k // CORES
    c = k % CORES
    oc = 1 - c
    partner = (z * CORES + oc, t)
    pending = []

    def send(src, dst, ssem, rsem, dev):
        cp = pltpu.make_async_remote_copy(
            src_ref=src, dst_ref=dst, send_sem=ssem, recv_sem=rsem, device_id=dev, device_id_type=MESH)
        cp.start()
        pending.append(cp)

    def arrived(dst, ssem, rsem):
        pltpu.make_async_remote_copy(
            src_ref=dst, dst_ref=dst, send_sem=ssem, recv_sem=rsem, device_id=partner,
            device_id_type=MESH).wait_recv()

    def load(src, dst, sem):
        cp = pltpu.make_async_copy(src, dst, sem)
        cp.start()
        return cp

    def cols(j):
        return pl.ds(j * FC, FC)

    sem_n = iter(range(64))
    pre_loads = []
    for j in range(nch):
        pre_loads.append([
            load(pg_h.at[:, cols(j)], wpg.at[:, cols(j)], w_sem.at[next(sem_n)]),
            load(pu_h.at[:, cols(j)], wpu.at[:, cols(j)], w_sem.at[next(sem_n)])])

    barrier = pltpu.get_barrier_semaphore()
    for d in range(1, NK):
        pl.semaphore_signal(barrier, inc=1, device_id=((k + d) % NK, t), device_id_type=MESH)
    for d in range(1, NT):
        pl.semaphore_signal(barrier, inc=1, device_id=(k, (t + d) % NT), device_id_type=MESH)
    pl.semaphore_wait(barrier, NK - 1 + NT - 1)

    if aligned:
        w_tok = tokens.shape[1]
        mine = pl.ds(pl.multiple_of(t * w_tok, w_tok), w_tok)
        for d in range(1, NT):
            send(tokens, x0.at[:, mine], tok_s.at[d - 1], tok_r.at[d - 1], (k, (t + d) % NT))
        x0[:, mine] = tokens[...]
        for d in range(1, NT):
            src = (t - d + NT) % NT
            arrived(x0.at[:, pl.ds(pl.multiple_of(src * w_tok, w_tok), w_tok)], tok_s.at[d - 1], tok_r.at[d - 1])
    else:
        x0[...] = tokens[...]

    def squares(x32, bufs):
        s_buf, r_buf, ss, rs = bufs
        ssq = jnp.sum(x32 * x32, axis=1, keepdims=True)
        s_buf[...] = jnp.broadcast_to(ssq, (ROWS, 128)).reshape(NK, RL, 128)
        for d in range(1, NK):
            peer = (k + d) % NK
            send(s_buf.at[peer], r_buf.at[d - 1], ss.at[d - 1], rs.at[d - 1], (peer, t))

    def row_scale(bufs):
        s_buf, r_buf, ss, rs = bufs
        total = s_buf[k]
        for d in range(1, NK):
            arrived(r_buf.at[d - 1], ss.at[d - 1], rs.at[d - 1])
            total = total + r_buf[d - 1]
        return lax.rsqrt(total[:, :1] / D + EPSILON)

    z_order = sorted(range(1, NZ), key=lambda d: -min(d, NZ - d))

    def reduce_start(j, a, s1, r1, e_s, e_r):
        s1[j] = a[j, :, :, oc].astype(BF16)
        send(s1.at[j], r1.at[j], e_s.at[j], e_r.at[j], partner)

    def reduce_middle(j, a, r1, s2, r2, e_s, e_r, z_s, z_r):
        arrived(r1.at[j], e_s.at[j], e_r.at[j])
        for d in z_order:
            zp = (z + d) % NZ
            s2[j, d - 1] = (a[j, :, zp, c] + r1[j, :, zp].astype(F32)).astype(BF16)
            send(s2.at[j, d - 1], r2.at[j, d - 1], z_s.at[j, d - 1], z_r.at[j, d - 1], (zp * CORES + c, t))

    def reduce_end(j, a, r1, r2, z_s, z_r):
        total = a[j, :, z, c] + r1[j, :, z].astype(F32)
        for d in range(1, NZ):
            arrived(r2.at[j, d - 1], z_s.at[j, d - 1], z_r.at[j, d - 1])
            total = total + r2[j, d - 1].astype(F32)
        return total

    def block(x32, gain, wg, wu, wd, gu_loads, d_loads, after, sq, bufs):
        a, s1, r1, s2, r2, hid, e_s, e_r, z_s, z_r, h_s, h_r, p_s, p_r = bufs
        squares(x32, sq)
        y = (x32 * gain[...]).astype(BF16)
        for j in range(nch):
            for cp in gu_loads[j]:
                cp.wait()
            if j == nch - 1:
                after()
            for g, w in enumerate((wg, wu)):
                prod = jnp.dot(y, w[:, cols(j)], preferred_element_type=F32)
                a[j, g] = prod.reshape(NZ, CORES, RL, FC)
            reduce_start(j, a, s1, r1, e_s, e_r)
        for j in range(nch):
            reduce_middle(j, a, r1, s2, r2, e_s, e_r, z_s, z_r)
        scale = row_scale(sq)
        for j in range(nch):
            total = reduce_end(j, a, r1, r2, z_s, z_r)
            hid[j, z, c] = (silu(total[0] * scale) * (total[1] * scale)).astype(BF16)
            own = hid.at[j, z, c]
            for d in z_order:
                send(own, own, h_s.at[j, d - 1], h_r.at[j, d - 1], (((z + d) % NZ) * CORES + c, t))
            send(own, own, p_s.at[j, 0], p_r.at[j, 0], partner)
        for j in range(nch):
            for d in reversed(z_order):
                src = hid.at[j, (z - d + NZ) % NZ, c]
                arrived(src, h_s.at[j, d - 1], h_r.at[j, d - 1])
                send(src, src, p_s.at[j, d], p_r.at[j, d], partner)
        part = None
        for j in range(nch):
            d_loads[j].wait()
            for d in range(NZ):
                arrived(hid.at[j, (z - d + NZ) % NZ, oc], p_s.at[j, d], p_r.at[j, d])
            h = hid[j].astype(F32).reshape(ROWS, FC).astype(BF16)
            term = jnp.dot(h, wd[pl.ds(j * FC, FC), :], preferred_element_type=F32)
            part = term if part is None else part + term
        return part

    def sum_tp(part, bufs):
        buf, ss, rs = bufs
        buf[t] = part.astype(BF16)
        for d in range(1, NT):
            send(buf.at[t], buf.at[t], ss.at[d - 1], rs.at[d - 1], (k, (t + d) % NT))
        for d in range(1, NT):
            arrived(buf.at[(t - d + NT) % NT], ss.at[d - 1], rs.at[d - 1])
        total = buf[0].astype(F32)
        for s in range(1, NT):
            total = total + buf[s].astype(F32)
        return total

    later = {}

    def start_later():
        later["pd"] = [load(pd_h.at[pl.ds(j * FC, FC)], wpd.at[pl.ds(j * FC, FC)], w_sem.at[next(sem_n)])
                       for j in range(nch)]
        later["q"] = [load(h, wq.at[n], w_sem.at[next(sem_n)]) for n, h in enumerate((q_h, f_h, i_h, o_h))]
        later["st"] = load(states_h, st, st_sem.at[0])
        later["mw"] = load(mw_h, wmw, w_sem.at[next(sem_n)])
        later["sgu"] = [[load(sg_h.at[:, cols(j)], wsg.at[:, cols(j)], w_sem.at[next(sem_n)]),
                         load(su_h.at[:, cols(j)], wsu.at[:, cols(j)], w_sem.at[next(sem_n)])]
                        for j in range(nch)]
        later["sd"] = [load(sd_h.at[pl.ds(j * FC, FC)], wsd.at[pl.ds(j * FC, FC)], w_sem.at[next(sem_n)])
                       for j in range(nch)]

    class Lazy:
        def __getitem__(self, j):
            return later["pd"][j]

    part = block(x0[...].astype(F32), g_pre, wpg, wpu, wpd, pre_loads, Lazy(), start_later, sq_bufs[0], ffn_bufs[0])
    total = sum_tp(part, ar_bufs[0])
    x1[...] = (x0[...].astype(F32) + 0.5 * total).astype(BF16)

    x32 = x1[...].astype(F32)
    a, s1, r1, s2, r2, e_s, e_r, z_s, z_r = mix_bufs
    squares(x32, sq_bufs[1])
    y = (x32 * g_mix[...]).astype(BF16)
    for g in range(4):
        later["q"][g].wait()
        a[0, g] = jnp.dot(y, wq[g], preferred_element_type=F32).reshape(NZ, CORES, RL, HL)
    reduce_start(0, a, s1, r1, e_s, e_r)
    reduce_middle(0, a, r1, s2, r2, e_s, e_r, z_s, z_r)
    scale = row_scale(sq_bufs[1])
    owned = reduce_end(0, a, r1, r2, z_s, z_r)
    queries = silu(owned[0] * scale)
    forget_raw = owned[1] * scale
    fresh = owned[2] * scale
    gates = silu(owned[3] * scale)
    nseq = RL // W
    row = lax.broadcasted_iota(jnp.int32, (RL, 1), 0)
    slot_len = jnp.zeros((RL, 1), jnp.int32)
    for s in range(nseq):
        slot_len = jnp.where(row // W == s, lengths[k * nseq + s], slot_len)
    live = (row % W) < slot_len
    fl = floor[...]
    forgets = jnp.where(live, fl + (1.0 - fl) * sigmoid(forget_raw), 1.0)
    later["st"].wait()
    for h in range(HL // DK):
        hs = slice(h * DK, (h + 1) * DK)
        f_t = forgets[:, hs].T
        q_t = queries[:, hs].T
        for s in range(nseq):
            carried = st[s, h]
            for o in range(W):
                r = s * W + o
                f_col = jnp.broadcast_to(f_t[:, r:r + 1], (DK, DK))
                carried = f_col * carried + (1.0 - f_col) * fresh[r:r + 1, hs]
                ro[r:r + 1, hs] = jnp.sum(q_t[:, r:r + 1] * carried, axis=0, keepdims=True)
            st[s, h] = carried
    st_out = load(st, ns_h, st_sem.at[1])
    live32 = live.astype(F32)
    hg, hg_s, hg_r = hg_bufs
    for h in range(HL // DK):
        hs = slice(h * DK, (h + 1) * DK)
        read = ro[:, hs]
        meansq = jnp.mean(read * read, axis=1, keepdims=True)
        hg[k, :, hs] = (read * lax.rsqrt(meansq + EPSILON) * head_gain[...] * gates[:, hs] * live32).astype(BF16)
    for d in range(1, NK):
        send(hg.at[k], hg.at[k], hg_s.at[d - 1], hg_r.at[d - 1], ((k + d) % NK, t))
    later["mw"].wait()
    for d in range(1, NK):
        arrived(hg.at[(k - d + NK) % NK], hg_s.at[d - 1], hg_r.at[d - 1])
    heads = hg[...].astype(F32).reshape(ROWS, HL).astype(BF16)
    total = sum_tp(jnp.dot(heads, wmw[...], preferred_element_type=F32), ar_bufs[1])
    x2[...] = (x1[...].astype(F32) + total).astype(BF16)

    part = block(x2[...].astype(F32), g_post, wsg, wsu, wsd, later["sgu"], later["sd"], lambda: None,
                 sq_bufs[2], ffn_bufs[1])
    buf, ss, rs = ar_bufs[2]
    if aligned:
        p_send, p_own = fin
        p_own[...] = part
        p_send[...] = part.astype(BF16)
        for d in range(1, NT):
            peer = (t + d) % NT
            send(p_send.at[:, pl.ds(pl.multiple_of(peer * w_tok, w_tok), w_tok)], buf.at[d - 1],
                 ss.at[d - 1], rs.at[d - 1], (k, peer))
        total = p_own[:, mine]
        for d in range(1, NT):
            arrived(buf.at[d - 1], ss.at[d - 1], rs.at[d - 1])
            total = total + buf[d - 1].astype(F32)
        out[...] = (x2[:, mine].astype(F32) + 0.5 * total).astype(BF16)
    else:
        total = sum_tp(part, ar_bufs[2])
        out[...] = (x2[...].astype(F32) + 0.5 * total).astype(BF16)
    for cp in pending:
        cp.wait_send()
    st_out.wait()


def local(NK, NT, tokens, lengths, states, gain_pre, pre_gate, pre_up, pre_down, gain_mix, query_weight,
          forget_weight, input_weight, outgate_weight, forget_floor, head_gain, mix_weight, gain_post, post_gate,
          post_up, post_down):
    ROWS, w_tok = tokens.shape
    C, FL = pre_gate.shape
    HL = query_weight.shape[1]
    NZ = NK // CORES
    RL = ROWS // NK
    aligned = w_tok % 128 == 0
    nch = 2 if FL % 256 == 0 else 1
    FC = FL // nch
    if not aligned:
        tokens = lax.all_gather(tokens, "tp", axis=1, tiled=True)
    vm = lambda shape, dt=BF16: pltpu.VMEM(shape, dt)
    sem = lambda *shape: pltpu.SemaphoreType.DMA(shape)
    scratch = [vm((ROWS, C))] * 3 + [
        vm((C, FL)), vm((C, FL)), vm((FL, C)), vm((4, C, HL)), vm((HL, C)), vm((C, FL)), vm((C, FL)), vm((FL, C)),
        vm(states.shape, F32), sem(NT - 1), sem(NT - 1), sem(6 * nch + 5), sem(2)]
    for _ in range(3):
        scratch += [vm((NK, RL, 128), F32), vm((NK - 1, RL, 128), F32), sem(NK - 1), sem(NK - 1)]
    for _ in range(2):
        scratch += [
            vm((nch, 2, NZ, CORES, RL, FC), F32), vm((nch, 2, NZ, RL, FC)), vm((nch, 2, NZ, RL, FC)),
            vm((nch, NZ - 1, 2, RL, FC)), vm((nch, NZ - 1, 2, RL, FC)), vm((nch, NZ, CORES, RL, FC)),
            sem(nch), sem(nch), sem(nch, NZ - 1), sem(nch, NZ - 1), sem(nch, NZ - 1), sem(nch, NZ - 1),
            sem(nch, NZ), sem(nch, NZ)]
    scratch += [
        vm((1, 4, NZ, CORES, RL, HL), F32), vm((1, 4, NZ, RL, HL)), vm((1, 4, NZ, RL, HL)),
        vm((1, NZ - 1, 4, RL, HL)), vm((1, NZ - 1, 4, RL, HL)),
        sem(1), sem(1), sem(1, NZ - 1), sem(1, NZ - 1)]
    scratch += [vm((NK, RL, HL)), sem(NK - 1), sem(NK - 1), vm((RL, HL), F32)]
    for _ in range(2):
        scratch += [vm((NT, ROWS, C)), sem(NT - 1), sem(NT - 1)]
    scratch += [vm((NT - 1, ROWS, w_tok)) if aligned else vm((NT, ROWS, C)), sem(NT - 1), sem(NT - 1)]
    scratch += [vm((ROWS, C)), vm((ROWS, C), F32)]
    V = pl.BlockSpec(memory_space=pltpu.VMEM)
    A = pl.BlockSpec(memory_space=pl.ANY)
    S = pl.BlockSpec(memory_space=pltpu.SMEM)
    ow = w_tok if aligned else C
    finished, new_states = pl.pallas_call(
        functools.partial(kernel, (NK, NT, C, FL, HL, ROWS, aligned, nch)),
        out_shape=(jax.ShapeDtypeStruct((ROWS, ow), BF16), jax.ShapeDtypeStruct(states.shape, F32)),
        in_specs=[V, S, A, V, A, A, A, V, A, A, A, A, V, V, A, V, A, A, A],
        out_specs=(V, A),
        scratch_shapes=scratch,
        compiler_params=pltpu.CompilerParams(
            collective_id=0, has_side_effects=True, vmem_limit_bytes=60 * 1024 * 1024),
    )(tokens, lengths, states, gain_pre[None], pre_gate, pre_up, pre_down, gain_mix[None], query_weight,
      forget_weight, input_weight, outgate_weight, forget_floor[None], head_gain[None], mix_weight, gain_post[None],
      post_gate, post_up, post_down)
    if not aligned:
        finished = lax.dynamic_slice_in_dim(finished, lax.axis_index("tp") * w_tok, w_tok, axis=1)
    live_rows = (jnp.arange(W, dtype=jnp.int32)[None, :] < lengths[:, None]).reshape(-1, 1)
    return jnp.where(live_rows, finished, jnp.zeros_like(finished)), new_states


def solution(mesh):
    placed = (
        P(None, ("kv", "tp")), P(), P("kv", "tp", None, None),
        P("kv"), P("kv", "tp"), P("kv", "tp"), P("tp", "kv"),
        P("kv"), P("kv", "tp"), P("kv", "tp"), P("kv", "tp"), P("kv", "tp"), P("tp"), P(), P("tp", "kv"),
        P("kv"), P("kv", "tp"), P("kv", "tp"), P("tp", "kv"),
    )
    return jax.shard_map(
        functools.partial(local, mesh.shape["kv"], mesh.shape["tp"]),
        mesh=mesh,
        in_specs=placed,
        out_specs=(P(None, ("kv", "tp")), P("kv", "tp", None, None)),
        check_vma=False,
    )
```

```python
import functools

import jax
import jax.numpy as jnp
from jax import lax
from jax.experimental import pallas as pl
from jax.experimental.pallas import tpu as pltpu
from jax.sharding import PartitionSpec as P

D = 4096
DK = 128
W = 4
EPSILON = 1e-06
MESH = pl.DeviceIdType.MESH
F32 = jnp.float32
BF16 = jnp.bfloat16
CORES = 2


def silu(v):
    return v / (1.0 + jnp.exp(-v))


def sigmoid(v):
    return 1.0 / (1.0 + jnp.exp(-v))


def kernel(cfg, *refs):
    NK, NT, C, FL, HL, ROWS, aligned, widths = cfg
    NZ = NK // CORES
    RL = ROWS // NK
    nch = len(widths)
    starts = [sum(widths[:j]) for j in range(nch)]
    it = iter(refs)
    (tokens, lengths, states_h, g_pre, pg_h, pu_h, pd_h, g_mix, q_h, f_h, i_h, o_h, floor, head_gain, mw_h,
     g_post, sg_h, su_h, sd_h) = [next(it) for _ in range(19)]
    out, ns_h = next(it), next(it)
    (x0, x1, x2, wpg, wpu, wpd, wq, wmw, wsg, wsu, wsd, st, tok_s, tok_r, w_sem, st_sem) = [
        next(it) for _ in range(16)]
    sq_bufs = [[next(it) for _ in range(4)] for _ in range(3)]
    ffn_bufs = [[[next(it) for _ in range(14)] for _ in range(nch)] for _ in range(2)]
    mix_bufs = [next(it) for _ in range(9)]
    hg_bufs = [next(it) for _ in range(3)]
    ro = next(it)
    ar_bufs = [[next(it) for _ in range(3)] for _ in range(3)]
    fin = [next(it) for _ in range(2)]

    k = lax.axis_index("kv")
    t = lax.axis_index("tp")
    z = k // CORES
    c = k % CORES
    oc = 1 - c
    partner = (z * CORES + oc, t)
    pending = []

    def send(src, dst, ssem, rsem, dev):
        cp = pltpu.make_async_remote_copy(
            src_ref=src, dst_ref=dst, send_sem=ssem, recv_sem=rsem, device_id=dev, device_id_type=MESH)
        cp.start()
        pending.append(cp)

    def arrived(dst, ssem, rsem):
        pltpu.make_async_remote_copy(
            src_ref=dst, dst_ref=dst, send_sem=ssem, recv_sem=rsem, device_id=partner,
            device_id_type=MESH).wait_recv()

    def load(src, dst, sem):
        cp = pltpu.make_async_copy(src, dst, sem)
        cp.start()
        return cp

    def cols(j):
        return pl.ds(starts[j], widths[j])

    sem_n = iter(range(64))
    pre_loads = []
    for j in range(nch):
        pre_loads.append([
            load(pg_h.at[:, cols(j)], wpg.at[:, cols(j)], w_sem.at[next(sem_n)]),
            load(pu_h.at[:, cols(j)], wpu.at[:, cols(j)], w_sem.at[next(sem_n)])])

    barrier = pltpu.get_barrier_semaphore()
    for d in range(1, NK):
        pl.semaphore_signal(barrier, inc=1, device_id=((k + d) % NK, t), device_id_type=MESH)
    for d in range(1, NT):
        pl.semaphore_signal(barrier, inc=1, device_id=(k, (t + d) % NT), device_id_type=MESH)
    pl.semaphore_wait(barrier, NK - 1 + NT - 1)

    if aligned:
        w_tok = tokens.shape[1]
        mine = pl.ds(pl.multiple_of(t * w_tok, w_tok), w_tok)
        for d in range(1, NT):
            send(tokens, x0.at[:, mine], tok_s.at[d - 1], tok_r.at[d - 1], (k, (t + d) % NT))
        x0[:, mine] = tokens[...]
        for d in range(1, NT):
            src = (t - d + NT) % NT
            arrived(x0.at[:, pl.ds(pl.multiple_of(src * w_tok, w_tok), w_tok)], tok_s.at[d - 1], tok_r.at[d - 1])
    else:
        x0[...] = tokens[...]

    def squares(x32, bufs):
        s_buf, r_buf, ss, rs = bufs
        ssq = jnp.sum(x32 * x32, axis=1, keepdims=True)
        s_buf[...] = jnp.broadcast_to(ssq, (ROWS, 128)).reshape(NK, RL, 128)
        for d in range(1, NK):
            peer = (k + d) % NK
            send(s_buf.at[peer], r_buf.at[d - 1], ss.at[d - 1], rs.at[d - 1], (peer, t))

    def row_scale(bufs):
        s_buf, r_buf, ss, rs = bufs
        total = s_buf[k]
        for d in range(1, NK):
            arrived(r_buf.at[d - 1], ss.at[d - 1], rs.at[d - 1])
            total = total + r_buf[d - 1]
        return lax.rsqrt(total[:, :1] / D + EPSILON)

    z_order = sorted(range(1, NZ), key=lambda d: -min(d, NZ - d))

    def two_terms(v):
        high = v.astype(BF16)
        return jnp.concatenate([high, (v - high.astype(F32)).astype(BF16)], axis=0)

    def two_term_dot(v, w):
        both = jnp.dot(v, w, preferred_element_type=F32)
        return both[:ROWS] + both[ROWS:]

    def reduce_start(bufs):
        a, s1, r1, s2, r2, e_s, e_r, z_s, z_r = bufs
        s1[...] = a[:, :, oc]
        send(s1, r1, e_s.at[0], e_r.at[0], partner)

    def reduce_middle(bufs):
        a, s1, r1, s2, r2, e_s, e_r, z_s, z_r = bufs
        arrived(r1, e_s.at[0], e_r.at[0])
        for d in z_order:
            zp = (z + d) % NZ
            s2[d - 1] = (a[:, zp, c] + r1[:, zp]).astype(BF16)
            send(s2.at[d - 1], r2.at[d - 1], z_s.at[d - 1], z_r.at[d - 1], (zp * CORES + c, t))

    def reduce_end(bufs):
        a, s1, r1, s2, r2, e_s, e_r, z_s, z_r = bufs
        total = a[:, z, c] + r1[:, z]
        for d in range(1, NZ):
            arrived(r2.at[d - 1], z_s.at[d - 1], z_r.at[d - 1])
            total = total + r2[d - 1].astype(F32)
        return total

    def block(x32, gain, wg, wu, wd, gu_loads, d_loads, after, sq, bufs):
        squares(x32, sq)
        y = two_terms(x32 * gain[...])
        for j in range(nch):
            for cp in gu_loads[j]:
                cp.wait()
            if j == nch - 1:
                after()
            for g, w in enumerate((wg, wu)):
                prod = two_term_dot(y, w[:, cols(j)])
                bufs[j][0][g] = prod.reshape(NZ, CORES, RL, widths[j])
            reduce_start(bufs[j][:9])
            if j:
                reduce_middle(bufs[j - 1][:9])
        reduce_middle(bufs[nch - 1][:9])
        scale = row_scale(sq)

        def forward(j):
            hid, h_s, h_r, p_s, p_r = bufs[j][9:]
            for d in reversed(z_order):
                src = hid.at[(z - d + NZ) % NZ, c]
                arrived(src, h_s.at[d - 1], h_r.at[d - 1])
                send(src, src, p_s.at[d], p_r.at[d], partner)

        def down(j):
            hid, h_s, h_r, p_s, p_r = bufs[j][9:]
            d_loads[j].wait()
            for d in range(NZ):
                arrived(hid.at[(z - d + NZ) % NZ, oc], p_s.at[d], p_r.at[d])
            h = hid[...].astype(F32).reshape(ROWS, widths[j]).astype(BF16)
            return jnp.dot(h, wd[cols(j), :], preferred_element_type=F32)

        for j in range(nch):
            hid, h_s, h_r, p_s, p_r = bufs[j][9:]
            total = reduce_end(bufs[j][:9])
            hid[z, c] = (silu(total[0] * scale) * (total[1] * scale)).astype(BF16)
            own = hid.at[z, c]
            for d in z_order:
                send(own, own, h_s.at[d - 1], h_r.at[d - 1], (((z + d) % NZ) * CORES + c, t))
            send(own, own, p_s.at[0], p_r.at[0], partner)
            if j >= 2:
                forward(j - 2)
        for j in range(max(nch - 2, 0), nch - 1):
            forward(j)
        part = None
        for j in range(nch):
            if j == min(1, nch - 1):
                forward(nch - 1)
            term = down(j)
            part = term if part is None else part + term
        return part

    def sum_tp(part, bufs):
        buf, ss, rs = bufs
        buf[t] = part.astype(BF16)
        for d in range(1, NT):
            send(buf.at[t], buf.at[t], ss.at[d - 1], rs.at[d - 1], (k, (t + d) % NT))
        for d in range(1, NT):
            arrived(buf.at[(t - d + NT) % NT], ss.at[d - 1], rs.at[d - 1])
        total = buf[0].astype(F32)
        for s in range(1, NT):
            total = total + buf[s].astype(F32)
        return total

    later = {}

    def start_later():
        later["pd"] = [load(pd_h.at[cols(j)], wpd.at[cols(j)], w_sem.at[next(sem_n)])
                       for j in range(nch)]
        later["q"] = [load(h, wq.at[n], w_sem.at[next(sem_n)]) for n, h in enumerate((q_h, f_h, i_h, o_h))]
        later["st"] = load(states_h, st, st_sem.at[0])
        later["mw"] = load(mw_h, wmw, w_sem.at[next(sem_n)])
        later["sgu"] = [[load(sg_h.at[:, cols(j)], wsg.at[:, cols(j)], w_sem.at[next(sem_n)]),
                         load(su_h.at[:, cols(j)], wsu.at[:, cols(j)], w_sem.at[next(sem_n)])]
                        for j in range(nch)]
        later["sd"] = [load(sd_h.at[cols(j)], wsd.at[cols(j)], w_sem.at[next(sem_n)])
                       for j in range(nch)]

    class Lazy:
        def __getitem__(self, j):
            return later["pd"][j]

    part = block(x0[...].astype(F32), g_pre, wpg, wpu, wpd, pre_loads, Lazy(), start_later, sq_bufs[0], ffn_bufs[0])
    total = sum_tp(part, ar_bufs[0])
    x1[...] = (x0[...].astype(F32) + 0.5 * total).astype(BF16)

    x32 = x1[...].astype(F32)
    squares(x32, sq_bufs[1])
    y = two_terms(x32 * g_mix[...])
    for g in range(4):
        later["q"][g].wait()
        mix_bufs[0][g] = two_term_dot(y, wq[g]).reshape(NZ, CORES, RL, HL)
    reduce_start(mix_bufs)
    reduce_middle(mix_bufs)
    scale = row_scale(sq_bufs[1])
    owned = reduce_end(mix_bufs)
    queries = silu(owned[0] * scale)
    forget_raw = owned[1] * scale
    fresh = owned[2] * scale
    gates = silu(owned[3] * scale)
    nseq = RL // W
    row = lax.broadcasted_iota(jnp.int32, (RL, 1), 0)
    slot_len = jnp.zeros((RL, 1), jnp.int32)
    for s in range(nseq):
        slot_len = jnp.where(row // W == s, lengths[k * nseq + s], slot_len)
    live = (row % W) < slot_len
    fl = floor[...]
    forgets = jnp.where(live, fl + (1.0 - fl) * sigmoid(forget_raw), 1.0)
    later["st"].wait()
    for h in range(HL // DK):
        hs = slice(h * DK, (h + 1) * DK)
        f_t = forgets[:, hs].T
        q_t = queries[:, hs].T
        for s in range(nseq):
            carried = st[s, h]
            for o in range(W):
                r = s * W + o
                f_col = jnp.broadcast_to(f_t[:, r:r + 1], (DK, DK))
                carried = f_col * carried + (1.0 - f_col) * fresh[r:r + 1, hs]
                ro[r:r + 1, hs] = jnp.sum(q_t[:, r:r + 1] * carried, axis=0, keepdims=True)
            st[s, h] = carried
    st_out = load(st, ns_h, st_sem.at[1])
    live32 = live.astype(F32)
    hg, hg_s, hg_r = hg_bufs
    for h in range(HL // DK):
        hs = slice(h * DK, (h + 1) * DK)
        read = ro[:, hs]
        meansq = jnp.mean(read * read, axis=1, keepdims=True)
        hg[k, :, hs] = (read * lax.rsqrt(meansq + EPSILON) * head_gain[...] * gates[:, hs] * live32).astype(BF16)
    for d in range(1, NK):
        send(hg.at[k], hg.at[k], hg_s.at[d - 1], hg_r.at[d - 1], ((k + d) % NK, t))
    later["mw"].wait()
    for d in range(1, NK):
        arrived(hg.at[(k - d + NK) % NK], hg_s.at[d - 1], hg_r.at[d - 1])
    heads = hg[...].astype(F32).reshape(ROWS, HL).astype(BF16)
    total = sum_tp(jnp.dot(heads, wmw[...], preferred_element_type=F32), ar_bufs[1])
    x2[...] = (x1[...].astype(F32) + total).astype(BF16)

    part = block(x2[...].astype(F32), g_post, wsg, wsu, wsd, later["sgu"], later["sd"], lambda: None,
                 sq_bufs[2], ffn_bufs[1])
    row = lax.broadcasted_iota(jnp.int32, (ROWS, 1), 0)
    row_len = jnp.zeros((ROWS, 1), jnp.int32)
    for s in range(ROWS // W):
        row_len = jnp.where(row // W == s, lengths[s], row_len)
    live_rows = ((row % W) < row_len).astype(F32)
    buf, ss, rs = ar_bufs[2]
    if aligned:
        p_send, p_own = fin
        p_own[...] = part
        p_send[...] = part.astype(BF16)
        for d in range(1, NT):
            peer = (t + d) % NT
            send(p_send.at[:, pl.ds(pl.multiple_of(peer * w_tok, w_tok), w_tok)], buf.at[d - 1],
                 ss.at[d - 1], rs.at[d - 1], (k, peer))
        total = p_own[:, mine]
        for d in range(1, NT):
            arrived(buf.at[d - 1], ss.at[d - 1], rs.at[d - 1])
            total = total + buf[d - 1].astype(F32)
        out[...] = ((x2[:, mine].astype(F32) + 0.5 * total) * live_rows).astype(BF16)
    else:
        total = sum_tp(part, ar_bufs[2])
        out[...] = ((x2[...].astype(F32) + 0.5 * total) * live_rows).astype(BF16)
    for cp in pending:
        cp.wait_send()
    st_out.wait()


def local(NK, NT, tokens, lengths, states, gain_pre, pre_gate, pre_up, pre_down, gain_mix, query_weight,
          forget_weight, input_weight, outgate_weight, forget_floor, head_gain, mix_weight, gain_post, post_gate,
          post_up, post_down):
    ROWS, w_tok = tokens.shape
    C, FL = pre_gate.shape
    HL = query_weight.shape[1]
    NZ = NK // CORES
    RL = ROWS // NK
    aligned = w_tok % 128 == 0
    tiles = FL // 256
    pieces = min(2, tiles)
    widths = (FL,) if FL % 256 else tuple(
        256 * (tiles // pieces + (1 if j < tiles % pieces else 0)) for j in range(pieces))
    nch = len(widths)
    if not aligned:
        tokens = lax.all_gather(tokens, "tp", axis=1, tiled=True)
    vm = lambda shape, dt=BF16: pltpu.VMEM(shape, dt)
    sem = lambda *shape: pltpu.SemaphoreType.DMA(shape)
    scratch = [vm((ROWS, C))] * 3 + [
        vm((C, FL)), vm((C, FL)), vm((FL, C)), vm((4, C, HL)), vm((HL, C)), vm((C, FL)), vm((C, FL)), vm((FL, C)),
        vm(states.shape, F32), sem(NT - 1), sem(NT - 1), sem(6 * nch + 5), sem(2)]
    for _ in range(3):
        scratch += [vm((NK, RL, 128), F32), vm((NK - 1, RL, 128), F32), sem(NK - 1), sem(NK - 1)]

    def reduce_bufs(parts, width):
        return [
            vm((parts, NZ, CORES, RL, width), F32), vm((parts, NZ, RL, width), F32), vm((parts, NZ, RL, width), F32),
            vm((NZ - 1, parts, RL, width)), vm((NZ - 1, parts, RL, width)),
            sem(1), sem(1), sem(NZ - 1), sem(NZ - 1)]

    for _ in range(2):
        for width in widths:
            scratch += reduce_bufs(2, width) + [
                vm((NZ, CORES, RL, width)), sem(NZ - 1), sem(NZ - 1), sem(NZ), sem(NZ)]
    scratch += reduce_bufs(4, HL)
    scratch += [vm((NK, RL, HL)), sem(NK - 1), sem(NK - 1), vm((RL, HL), F32)]
    for _ in range(2):
        scratch += [vm((NT, ROWS, C)), sem(NT - 1), sem(NT - 1)]
    scratch += [vm((NT - 1, ROWS, w_tok)) if aligned else vm((NT, ROWS, C)), sem(NT - 1), sem(NT - 1)]
    scratch += [vm((ROWS, C)), vm((ROWS, C), F32)]
    V = pl.BlockSpec(memory_space=pltpu.VMEM)
    A = pl.BlockSpec(memory_space=pl.ANY)
    S = pl.BlockSpec(memory_space=pltpu.SMEM)
    ow = w_tok if aligned else C
    finished, new_states = pl.pallas_call(
        functools.partial(kernel, (NK, NT, C, FL, HL, ROWS, aligned, widths)),
        out_shape=(jax.ShapeDtypeStruct((ROWS, ow), BF16), jax.ShapeDtypeStruct(states.shape, F32)),
        in_specs=[V, S, A, V, A, A, A, V, A, A, A, A, V, V, A, V, A, A, A],
        out_specs=(V, A),
        scratch_shapes=scratch,
        compiler_params=pltpu.CompilerParams(
            collective_id=0, has_side_effects=True, vmem_limit_bytes=60 * 1024 * 1024),
    )(tokens, lengths, states, gain_pre[None], pre_gate, pre_up, pre_down, gain_mix[None], query_weight,
      forget_weight, input_weight, outgate_weight, forget_floor[None], head_gain[None], mix_weight, gain_post[None],
      post_gate, post_up, post_down)
    if not aligned:
        finished = lax.dynamic_slice_in_dim(finished, lax.axis_index("tp") * w_tok, w_tok, axis=1)
    return finished, new_states


def solution(mesh):
    placed = (
        P(None, ("kv", "tp")), P(), P("kv", "tp", None, None),
        P("kv"), P("kv", "tp"), P("kv", "tp"), P("tp", "kv"),
        P("kv"), P("kv", "tp"), P("kv", "tp"), P("kv", "tp"), P("kv", "tp"), P("tp"), P(), P("tp", "kv"),
        P("kv"), P("kv", "tp"), P("kv", "tp"), P("tp", "kv"),
    )
    return jax.shard_map(
        functools.partial(local, mesh.shape["kv"], mesh.shape["tp"]),
        mesh=mesh,
        in_specs=placed,
        out_specs=(P(None, ("kv", "tp")), P("kv", "tp", None, None)),
        check_vma=False,
    )
```
